32 devices in a mesh: sp: 16 (over z, y, x), tp: 2 (over core).
Axes of the slice: x: 2, y: 2, z: 4, core: 2. Of those that a mesh axis runs over, the one named last changes fastest.
Arguments:
- tokens: bfloat16 [2048, 1024], P('sp', 'tp'), may hold values from -6 to 6
- norm_gain: float32 [1024], P('tp'), may hold values from 0.1 to 1.9
- query_weight: bfloat16 [1024, 1024], P('sp', 'tp'), may hold values from -0.1875 to 0.1875
- key_weight: bfloat16 [1024, 512], P('sp', 'tp'), may hold values from -0.1875 to 0.1875
- value_weight: bfloat16 [1024, 512], P('sp', 'tp'), may hold values from -0.1875 to 0.1875
- conv_in_weight: bfloat16 [1024, 1024], P('sp', 'tp'), may hold values from -0.1875 to 0.1875
- pre_weight: bfloat16 [1024, 1024], P('sp', 'tp'), may hold values from -0.1875 to 0.1875
- post_weight: bfloat16 [1024, 1024], P('sp', 'tp'), may hold values from -0.1875 to 0.1875
- attn_gate_weight: bfloat16 [1024, 1024], P('sp', 'tp'), may hold values from -0.1875 to 0.1875
- conv_gate_weight: bfloat16 [1024, 1024], P('sp', 'tp'), may hold values from -0.1875 to 0.1875
- sink_logit: float32 [16], P('tp'), may hold values from 1 to 5
- conv_taps: float32 [3, 1024], P(None, 'tp'), may hold values from -3 to 3
- attn_out_weight: bfloat16 [1024, 1024], P('tp', 'sp'), may hold values from -1 to 1
- conv_out_weight: bfloat16 [1024, 1024], P('tp', 'sp'), may hold values from -0.1875 to 0.1875
Outputs:
- merged: bfloat16 [2048, 1024], P('sp', 'tp')
The draws below stay inside these ranges and needn't reach their ends.
All inputs are finite; a program needn't handle non-finite values.
Results may differ from the reference program's by a relative error of at most 0.003.
Values may be sent and summed in bfloat16 or wider, within the bound.
A program may use at most 64 MiB of HBM per device.

```python
import jax
import jax.numpy as jnp
from jax import lax

D = 1024
Q_HEADS = 16
KV_HEADS = 8
HEAD_DIM = 64
WINDOW = 64
TOK_DEV = 128
GROUP = 2
ATTN_WIDTH = 1024
KV_WIDTH = 512
TOKENS = 2048


def steps_of(rng, extent, pieces, low, top_value):
    level, own = 1.0, jax.random.fold_in(rng, 6)
    for position, parts in pieces:
        heights = jnp.exp(jax.random.uniform(jax.random.fold_in(own, position), (parts,), jnp.float32, low / len(pieces), top_value / len(pieces)))
        level = level * jnp.repeat(heights, extent[position] // parts).reshape([-1 if axis == position else 1 for axis in range(len(extent))])
    return level


def centred(rng, shape, width, limit, shards=(), kind=jnp.bfloat16):
    result = jax.random.normal(rng, shape, jnp.float32) * width
    if len(shards) > 0:
        result = steps_of(rng, shape, shards, -0.22, 0.18) * result
    return jnp.clip(result, min=-limit, max=limit).astype(kind)


def setup_inputs(seed: int = 0) -> dict:
    arg_keys = jax.random.split(jax.random.key(seed), 15)
    return {
        "tokens": centred(arg_keys[0], (TOKENS, D), 1.0, 6.0, ((0, 16), (1, 2))),
        "norm_gain": jnp.clip(1.0 + 0.18 * jax.random.normal(arg_keys[1], (D,), jnp.float32), 0.1, 1.9),
        "query_weight": centred(arg_keys[2], (D, ATTN_WIDTH), D ** -0.5, 0.1875, ((0, 16), (1, 2))),
        "key_weight": centred(arg_keys[3], (D, KV_WIDTH), D ** -0.5, 0.1875, ((0, 16), (1, 2))),
        "value_weight": centred(arg_keys[4], (D, KV_WIDTH), D ** -0.5, 0.1875, ((0, 16), (1, 2))),
        "conv_in_weight": centred(arg_keys[5], (D, D), D ** -0.5, 0.1875, ((0, 16), (1, 2))),
        "pre_weight": centred(arg_keys[6], (D, D), D ** -0.5, 0.1875, ((0, 16), (1, 2))),
        "post_weight": centred(arg_keys[7], (D, D), D ** -0.5, 0.1875, ((0, 16), (1, 2))),
        "attn_gate_weight": centred(arg_keys[8], (D, D), D ** -0.5, 0.1875, ((0, 16), (1, 2))),
        "conv_gate_weight": centred(arg_keys[9], (D, D), D ** -0.5, 0.1875, ((0, 16), (1, 2))),
        "sink_logit": jnp.clip(1.0 + 4.0 * jax.random.uniform(arg_keys[10], (Q_HEADS,), jnp.float32) ** steps_of(arg_keys[10], (Q_HEADS,), ((0, 2),), -0.2, 0.2), 1.0, 5.0),
        "conv_taps": centred(arg_keys[11], (3, D), 0.577, 3.0, ((1, 2),), jnp.float32),
        "attn_out_weight": centred(arg_keys[12], (ATTN_WIDTH, D), (ATTN_WIDTH // 32) ** -0.5, 1.0, ((0, 2), (1, 16))),
        "conv_out_weight": centred(arg_keys[13], (D, D), D ** -0.5, 0.1875, ((0, 2), (1, 16))),
    }


epsilon = 1e-06
negative = -1e+30

def window_mix(queries, key_rows, value_rows, sink_cols, first, seq_total):
    score_scale = queries.shape[-1] ** (-0.5)
    scores = jnp.einsum('qhgd,khd->hgqk', queries, key_rows, precision=lax.Precision.HIGHEST) * score_scale
    qpos = first + jnp.arange(queries.shape[0], dtype=jnp.int32)
    kpos = first - WINDOW + jnp.arange(key_rows.shape[0], dtype=jnp.int32)
    allowed = (jnp.abs(qpos[:, None] - kpos[None, :]) <= WINDOW) & (kpos >= 0)[None, :] & (kpos < seq_total)[None, :]
    scores = jnp.where(allowed, scores, negative)
    column = jnp.broadcast_to(sink_cols[:, :, None, None], scores.shape[:-1] + (1,))
    weights_soft = jax.nn.softmax(jnp.concatenate([scores, column], axis=-1), axis=-1)[..., :-1]
    return jnp.einsum('hgqk,khd->qhgd', weights_soft, value_rows, precision=lax.Precision.HIGHEST)

def attention(queries, key_rows, value_rows, sink_logit):
    padding = ((WINDOW, WINDOW), (0, 0))
    key_pad = jnp.pad(key_rows.astype(jnp.float32), padding)
    value_pad = jnp.pad(value_rows.astype(jnp.float32), padding)
    span_rows = TOK_DEV + 2 * WINDOW
    sink_cols = sink_logit.reshape(KV_HEADS, GROUP)

    def block(block_index):
        first = block_index * TOK_DEV
        q_block = lax.dynamic_slice_in_dim(queries, first, TOK_DEV, 0).astype(jnp.float32)
        q_block = q_block.reshape(TOK_DEV, KV_HEADS, GROUP, HEAD_DIM)
        k_block = lax.dynamic_slice_in_dim(key_pad, first, span_rows, 0).reshape(span_rows, KV_HEADS, HEAD_DIM)
        v_block = lax.dynamic_slice_in_dim(value_pad, first, span_rows, 0).reshape(span_rows, KV_HEADS, HEAD_DIM)
        mixed_rows = window_mix(q_block, k_block, v_block, sink_cols, first, TOKENS)
        return mixed_rows.reshape(TOK_DEV, ATTN_WIDTH)
    blocks_out = lax.map(block, jnp.arange(TOKENS // TOK_DEV, dtype=jnp.int32))
    return blocks_out.reshape(TOKENS, ATTN_WIDTH).astype(jnp.bfloat16)

def reference(tokens, norm_gain, query_weight, key_weight, value_weight, conv_in_weight, pre_weight, post_weight, attn_gate_weight, conv_gate_weight, sink_logit, conv_taps, attn_out_weight, conv_out_weight):
    widened = tokens.astype(jnp.float32)
    mean_sq = lax.optimization_barrier(jnp.mean(widened * widened, axis=1, keepdims=True))
    normed = (widened * lax.rsqrt(mean_sq + epsilon) * norm_gain[None, :]).astype(jnp.bfloat16)

    def project(weight):
        return jnp.dot(normed, weight, preferred_element_type=jnp.float32)
    queries = project(query_weight).astype(jnp.bfloat16)
    key_rows = project(key_weight).astype(jnp.bfloat16)
    value_rows = project(value_weight).astype(jnp.bfloat16)
    conv_in = project(conv_in_weight).astype(jnp.bfloat16)
    pre_gate = project(pre_weight).astype(jnp.bfloat16)
    post_gate = project(post_weight).astype(jnp.bfloat16)
    attn_gate = project(attn_gate_weight)
    conv_gate = project(conv_gate_weight)
    attended = attention(queries, key_rows, value_rows, sink_logit)
    conv_mix = (pre_gate.astype(jnp.float32) * conv_in.astype(jnp.float32)).astype(jnp.bfloat16)
    padded = jnp.pad(conv_mix.astype(jnp.float32), ((1, 1), (0, 0)))
    convolved = conv_taps[0][None, :] * padded[:-2] + conv_taps[1][None, :] * padded[1:-1] + conv_taps[2][None, :] * padded[2:]
    conv_out = (post_gate.astype(jnp.float32) * convolved).astype(jnp.bfloat16)
    branch_attn = jnp.dot(attended, attn_out_weight, preferred_element_type=jnp.float32)
    branch_conv = jnp.dot(conv_out, conv_out_weight, preferred_element_type=jnp.float32)
    return (jax.nn.sigmoid(attn_gate) * branch_attn + jax.nn.sigmoid(conv_gate) * branch_conv).astype(jnp.bfloat16)
```

```python
import functools

import jax
import jax.numpy as jnp
from jax import lax
from jax.experimental import pallas as pl
from jax.experimental.pallas import tpu as pltpu
from jax.sharding import PartitionSpec as P

HEAD_DIM = 64
WINDOW = 64


epsilon = 1e-06
negative = -1e30


def folded(shard, axis, dim, absorb, state):
    everything = jax.tree.map(lambda a: lax.all_gather(a, axis, axis=dim, tiled=True), shard)
    return absorb(state, everything, jnp.int32(0))


def for_sending(shard):
    def short(part):
        return part.astype(jnp.bfloat16) if part.dtype == jnp.float32 else part

    return jax.tree.map(short, shard)


def extended(shard, sides, width, wrap):
    for axis, dim in sides:
        devices, length = lax.axis_size(axis), shard.shape[dim]
        up = [(i, (i + 1) % devices) for i in range(devices if wrap else devices - 1)]
        down = [(j, i) for i, j in up]
        last = lax.slice_in_dim(shard, length - width, length, axis=dim)
        first = lax.slice_in_dim(shard, 0, width, axis=dim)
        before = lax.ppermute(last, axis, up)
        after = lax.ppermute(first, axis, down)
        shard = jnp.concatenate([before, shard, after], axis=dim)
    return shard


def summed_rows(product, width, axis):
    whole = product(jnp.int32(0), width * lax.axis_size(axis))
    return lax.psum_scatter(whole, axis, scatter_dimension=0, tiled=True)


def window_mix(queries, key_rows, value_rows, sink_cols, first, seq_total):
    score_scale = queries.shape[-1] ** (-0.5)
    scores = (
        jnp.einsum("qhgd,khd->hgqk", queries, key_rows, preferred_element_type=jnp.float32)
        * score_scale
    )
    qpos = first + jnp.arange(queries.shape[0], dtype=jnp.int32)
    kpos = first - WINDOW + jnp.arange(key_rows.shape[0], dtype=jnp.int32)
    allowed = (
        (jnp.abs(qpos[:, None] - kpos[None, :]) <= WINDOW)
        & (kpos >= 0)[None, :]
        & (kpos < seq_total)[None, :]
    )
    scores = jnp.where(allowed, scores, negative)
    column = jnp.broadcast_to(sink_cols[:, :, None, None], scores.shape[:-1] + (1,))
    weights_soft = jax.nn.softmax(jnp.concatenate([scores, column], axis=-1), axis=-1)[..., :-1]
    return jnp.einsum(
        "hgqk,khd->qhgd",
        weights_soft,
        value_rows.astype(jnp.float32),
        precision=lax.Precision.HIGHEST,
    )


def short_conv(padded, conv_taps):
    return (
        conv_taps[0][None, :] * padded[:-2]
        + conv_taps[1][None, :] * padded[1:-1]
        + conv_taps[2][None, :] * padded[2:]
    )


def gathered_everywhere(
    tokens,
    norm_gain,
    query_weight,
    key_weight,
    value_weight,
    conv_in_weight,
    pre_weight,
    post_weight,
    attn_gate_weight,
    conv_gate_weight,
    sink_logit,
    conv_taps,
    attn_out_weight,
    conv_out_weight,
):
    tok_rows = tokens.shape[0]
    widened = tokens.astype(jnp.float32)
    row_sums = lax.psum(jnp.sum(widened * widened, axis=1), "tp")
    features = tokens.shape[1] * lax.axis_size("tp")
    normed = (
        widened * lax.rsqrt(row_sums[:, None] / features + epsilon) * norm_gain[None, :]
    ).astype(jnp.bfloat16)
    collected = (
        lax.all_gather(query_weight, "sp", axis=0, tiled=True),
        lax.all_gather(key_weight, "sp", axis=0, tiled=True),
        lax.all_gather(value_weight, "sp", axis=0, tiled=True),
        lax.all_gather(conv_in_weight, "sp", axis=0, tiled=True),
        lax.all_gather(pre_weight, "sp", axis=0, tiled=True),
        lax.all_gather(post_weight, "sp", axis=0, tiled=True),
        lax.all_gather(attn_gate_weight, "sp", axis=0, tiled=True),
        lax.all_gather(conv_gate_weight, "sp", axis=0, tiled=True),
    )
    stacked = jnp.concatenate(collected, axis=1)

    def add_rows(carry_sum, segment, first):
        rows_here = lax.dynamic_slice_in_dim(stacked, first, segment.shape[1], 0)
        return carry_sum + jnp.dot(segment, rows_here, preferred_element_type=jnp.float32)

    projected = folded(
        normed, "tp", 1, add_rows, jnp.zeros((tok_rows, stacked.shape[1]), jnp.float32)
    )
    pieces = []
    offset = 0
    for weight in collected:
        pieces.append(projected[:, offset : offset + weight.shape[1]])
        offset = offset + weight.shape[1]
    queries, key_rows, value_rows, conv_in, pre_gate, post_gate = [
        part_rows.astype(jnp.bfloat16) for part_rows in pieces[:6]
    ]
    attn_gate = pieces[6]
    conv_gate = pieces[7]
    conv_mix = (pre_gate.astype(jnp.float32) * conv_in.astype(jnp.float32)).astype(jnp.bfloat16)
    kv_width = key_rows.shape[1]
    kv_pad = extended(
        for_sending(jnp.concatenate([key_rows, value_rows], axis=1)), (("sp", 0),), WINDOW, False
    )
    key_pad = kv_pad[:, :kv_width]
    value_pad = kv_pad[:, kv_width:]
    conv_pad = extended(conv_mix, (("sp", 0),), 1, False)
    kv_local = kv_width // HEAD_DIM
    group_size = queries.shape[1] // kv_width
    first_row = lax.axis_index("sp") * tok_rows
    attended = window_mix(
        queries.reshape(tok_rows, kv_local, group_size, HEAD_DIM),
        key_pad.reshape(-1, kv_local, HEAD_DIM),
        value_pad.reshape(-1, kv_local, HEAD_DIM),
        sink_logit.reshape(kv_local, group_size),
        first_row,
        tok_rows * lax.axis_size("sp"),
    )
    attended = attended.reshape(tok_rows, -1).astype(jnp.bfloat16)
    conv_out = (
        post_gate.astype(jnp.float32) * short_conv(conv_pad.astype(jnp.float32), conv_taps)
    ).astype(jnp.bfloat16)
    attn_full, conv_full = (
        lax.all_gather(attn_out_weight, "sp", axis=1, tiled=True),
        lax.all_gather(conv_out_weight, "sp", axis=1, tiled=True),
    )

    def attn_term(first, number):
        columns = lax.dynamic_slice_in_dim(attn_full, first, number, 1)
        return jnp.dot(attended, columns, preferred_element_type=jnp.float32).T

    def conv_term(first, number):
        columns = lax.dynamic_slice_in_dim(conv_full, first, number, 1)
        return jnp.dot(conv_out, columns, preferred_element_type=jnp.float32).T

    out_rows = attn_gate.shape[1]

    def both_terms(first, number):
        return jnp.concatenate([attn_term(first, number), conv_term(first, number)], axis=1)

    summed = summed_rows(both_terms, out_rows, "tp")
    branch_attn = summed[:, :tok_rows].T
    branch_conv = summed[:, tok_rows:].T
    return (
        jax.nn.sigmoid(attn_gate) * branch_attn + jax.nn.sigmoid(conv_gate) * branch_conv
    ).astype(jnp.bfloat16)


MESH = pl.DeviceIdType.MESH
BF = jnp.bfloat16
F32 = jnp.float32


class Plan:
    def __init__(self, sp, tp, tokens, query, key, attn_out):
        self.sp, self.tp = sp, tp
        self.rows, self.feat = tokens.shape
        self.members = key.shape[1] // HEAD_DIM
        self.planes = sp // max(self.members, 1)
        self.depth = query.shape[0]
        self.q = query.shape[1] // max(self.members, 1)
        self.group = query.shape[1] // max(key.shape[1], 1)
        self.wide = attn_out.shape[1]
        self.pieces = self.q // max(self.wide, 1)
        self.all_rows = self.members * self.rows

    def fits(self):
        m = self.members
        return (
            tuple((self.tp, m > 1, self.planes > 1)) == (2, True, True)
            and self.sp == m * self.planes
            and self.q == 2 * HEAD_DIM
            and self.q % 128 == 0
            and self.feat == m * self.q
            and self.rows == 2 * WINDOW
            and self.depth % 16 == 0
            and self.pieces * self.wide == self.q
            and self.pieces * m * self.tp == self.sp
        )


def kernel(
    pl_, tokens_ref, gain_ref, pa_ref, pb_ref, po_ref, sink_ref, taps_ref, o_ref,
    tok, normed, gain, wa, wb, wo, woa, woc, qb, kvc, postb, act, gates, mix, outb,
    sends, recvs, local,
):
    M, G, T = pl_.members, pl_.planes, pl_.tp
    R, F, Q, DP = pl_.rows, pl_.feat, pl_.q, pl_.depth
    H, ALL = WINDOW, pl_.all_rows
    sp, c = lax.axis_index("sp"), lax.axis_index("tp")
    g, j = sp // M, lax.rem(sp, M)
    peer = 1 - c

    others = pl_.sp * T
    me = sp * T + c
    barrier = pltpu.get_barrier_semaphore()
    for d in range(1, others):
        t = lax.rem(me + d, others)
        pl.semaphore_signal(barrier, inc=1, device_id=(t // T, lax.rem(t, T)), device_id_type=MESH)
    pl.semaphore_wait(barrier, others - 1)

    base = {}
    top = 0
    for name, count in (
        ("tok", M), ("lo", 1), ("hi", 1), ("tok2", M), ("lo2", 1), ("hi2", 1), ("gain", 1),
        ("a", M), ("az", G), ("b", M), ("bz", G), ("wo", pl_.pieces * T),
        ("act", 2 * M), ("act2", 2 * M), ("out", M),
    ):
        base[name] = top
        top += count
    waits = []

    def arrived(dst, index):
        pltpu.make_async_remote_copy(
            src_ref=dst, dst_ref=dst, send_sem=sends.at[0], recv_sem=recvs.at[index],
            device_id=(sp, peer), device_id_type=MESH,
        ).wait_recv()

    def send(src, dst, index, to_sp, to_tp, when=None):
        copy = pltpu.make_async_remote_copy(
            src_ref=src, dst_ref=dst, send_sem=sends.at[len(waits)], recv_sem=recvs.at[index],
            device_id=(to_sp, to_tp), device_id_type=MESH,
        )
        waits.append((copy, when))
        if when is None:
            copy.start()
        else:
            pl.when(when)(lambda: copy.start())

    def al(x, n):
        return pl.multiple_of(x, n)

    def tok_at(member, half):
        return tok.at[pl.ds(al(H + member * R, 64), R), pl.ds(al(half * F, 128), F)]

    def lo_at(half):
        return tok.at[pl.ds(0, H), pl.ds(al(half * F, 128), F)]

    def hi_at(half):
        return tok.at[pl.ds(H + ALL, H), pl.ds(al(half * F, 128), F)]

    own_copies = []

    def keep(src, dst):
        copy = pltpu.make_async_copy(src, dst, local.at[len(own_copies)])
        copy.start()
        own_copies.append(copy)
        return copy

    for k in range(1, M):
        send(tokens_ref, tok_at(j, c), base["tok"] + j, g * M + lax.rem(j + k, M), c)
    send(tokens_ref, tok_at(j, c), base["tok2"] + j, sp, peer)
    gain_at = lambda half: gain.at[:, pl.ds(al(half * F, 128), F)]
    send(gain_ref, gain_at(c), base["gain"], sp, peer)
    up, down = lax.rem(g + 1, G), lax.rem(g + G - 1, G)
    for k in range(M):
        send(tokens_ref.at[pl.ds(R - H, H)], lo_at(c), base["lo"], up * M + k, c, j == M - 1)
        send(tokens_ref.at[pl.ds(0, H)], hi_at(c), base["hi"], down * M + k, c, j == 0)
    own_tok = keep(tokens_ref, tok_at(j, c))
    own_gain = keep(gain_ref, gain_at(c))

    def slot(w, plane, member):
        return w.at[pl.ds(al((plane * M + member) * DP, 16), DP)]

    def block(w, plane):
        return w.at[pl.ds(al(plane * M * DP, 16), M * DP)]

    def in_plane(w, packed, name):
        for k in range(1, M):
            to = lax.rem(j + k, M)
            send(packed.at[to], slot(w, g, j), base[name] + j, g * M + to, c)
        return keep(packed.at[j], slot(w, g, j))

    def own_block(w, name, copy):
        copy.wait()
        for k in range(1, M):
            source = lax.rem(j + M - k, M)
            arrived(slot(w, g, source), base[name] + source)
        pass_on(w, name, 0)

    def pass_on(w, name, d):
        low, high = lax.max(g - d, 0), lax.min(g + d, G - 1)
        if d > 0:
            pl.when(g - d >= 0)(lambda: arrived(block(w, low), base[name + "z"] + low))
        if d < G - 1:
            send(block(w, low), block(w, low), base[name + "z"] + low,
                 lax.min(g + 1, G - 1) * M + j, c, (g - d >= 0) & (g < G - 1))
        if d > 0:
            pl.when(g + d < G)(lambda: arrived(block(w, high), base[name + "z"] + high))
        if d < G - 1:
            send(block(w, high), block(w, high), base[name + "z"] + high,
                 lax.max(g - 1, 0) * M + j, c, (g + d < G) & (g > 0))

    keep_a = in_plane(wa, pa_ref, "a")
    keep_b = in_plane(wb, pb_ref, "b")
    own_block(wa, "a", keep_a)

    for k in range(1, M):
        source = lax.rem(j + M - k, M)
        arrived(tok_at(source, c), base["tok"] + source)
        send(tok_at(source, c), tok_at(source, c), base["tok2"] + source, sp, peer)
    arrived(lo_at(c), base["lo"])
    send(lo_at(c), lo_at(c), base["lo2"], sp, peer)
    arrived(hi_at(c), base["hi"])
    send(hi_at(c), hi_at(c), base["hi2"], sp, peer)
    own_tok.wait()
    own_gain.wait()
    arrived(gain_at(peer), base["gain"])
    for k in range(M):
        arrived(tok_at(k, peer), base["tok2"] + k)
    arrived(lo_at(peer), base["lo2"])
    arrived(hi_at(peer), base["hi2"])

    def norm(step, carry):
        at = pl.ds(al(step * H, 64), H)
        x = tok[at, :].astype(F32)
        mean = jnp.sum(x * x, axis=1, keepdims=True) / x.shape[1]
        normed[at, :] = (x * lax.rsqrt(mean + epsilon) * gain[...]).astype(BF)
        return carry

    lax.fori_loop(0, (ALL + 2 * H) // H, norm, 0)

    for d in range(1, G - 1):
        pass_on(wa, "a", d)
    own_block(wb, "b", keep_b)

    chunk = sp // pl_.pieces
    piece = lax.rem(sp, pl_.pieces)
    to_c, to_j = chunk // M, lax.rem(chunk, M)
    wo_at = lambda i, half: wo.at[i, pl.ds(al(half * F, 128), F)]
    mine = (to_c == c) & (to_j == j)
    for k in range(G):
        to = lax.rem(g + k, G) * M + to_j
        index = base["wo"] + piece * T + c
        send(po_ref, wo_at(piece, c), index, to, to_c, None if k else jnp.logical_not(mine))
    own_wo = pltpu.make_async_copy(po_ref, wo_at(piece, c), recvs.at[base["wo"] + piece * T + c])
    pl.when(mine)(lambda: own_wo.start())

    pass_on(wa, "a", G - 1)

    def kv_conv(p):
        kv = p[:, :Q].astype(BF)
        conv = (p[:, 2 * Q:3 * Q].astype(BF).astype(F32) * p[:, Q:2 * Q].astype(BF).astype(F32))
        return kv, conv.astype(BF)

    for at, inside in ((0, g > 0), (H + ALL, g < G - 1)):
        p = jnp.dot(normed[at:at + H, :], wa[:, Q:4 * Q], preferred_element_type=F32)
        p = jnp.where(inside, p, 0.0)
        kv, conv = kv_conv(p)
        kvc[at:at + H, :Q] = kv
        kvc[at:at + H, Q:] = conv

    def project(m, carry):
        p = jnp.dot(normed[pl.ds(al(H + m * R, 64), R), :], wa[...], preferred_element_type=F32)
        kv, conv = kv_conv(p[:, Q:4 * Q])
        at = pl.ds(al(H + m * R, 64), R)
        kvc[at, :Q] = kv
        kvc[at, Q:] = conv
        here = pl.ds(al(m * R, 128), R)
        qb[here, :] = p[:, :Q].astype(BF)
        postb[here, :] = p[:, 4 * Q:].astype(BF)
        return carry

    lax.fori_loop(0, M, project, 0)

    for d in range(1, G):
        pass_on(wb, "b", d)

    span = R + 2 * H
    own = c * M + j
    act_at = lambda branch, half, member: act.at[
        :, pl.ds(al(branch * T * F + half * F + member * Q, 128), Q)
    ]
    qi = lax.broadcasted_iota(jnp.int32, (R, span), 0)
    ki = lax.broadcasted_iota(jnp.int32, (R, span), 1)
    near = jnp.abs(ki - H - qi) <= H
    taps = taps_ref[:, pl.ds(al(j * Q, 128), Q)]

    def attend(m, carry):
        here = pl.ds(al(m * R, 128), R)
        keys = kvc[pl.ds(al(m * R, 64), span), :Q]
        k_rows, v_rows = keys[:, :HEAD_DIM], keys[:, HEAD_DIM:]
        kpos = g * ALL + m * R - H + ki
        allowed = near & (kpos >= 0) & (kpos < G * ALL)
        queries = qb[here, :]
        heads = []
        for h in range(pl_.group):
            q = queries[:, h * HEAD_DIM:(h + 1) * HEAD_DIM]
            s = lax.dot_general(q, k_rows, (((1,), (1,)), ((), ())), preferred_element_type=F32)
            s = jnp.where(allowed, s * HEAD_DIM ** -0.5, negative)
            sink = sink_ref[0, j * pl_.group + h]
            high = jnp.maximum(jnp.max(s, axis=1, keepdims=True), sink)
            e = jnp.exp(s - high)
            total = jnp.sum(e, axis=1, keepdims=True) + jnp.exp(sink - high)
            big = e.astype(BF)
            small = (e - big.astype(F32)).astype(BF)
            o = jnp.dot(big, v_rows, preferred_element_type=F32)
            o = o + jnp.dot(small, v_rows, preferred_element_type=F32)
            heads.append(o / total)
        act[here, pl.ds(al(own * Q, 128), Q)] = jnp.concatenate(heads, axis=1).astype(BF)
        x = kvc[pl.ds(al(m * R + H - 16, 16), R + 32), Q:].astype(F32)
        before = pltpu.roll(x, 1, 0)[16:16 + R]
        after = pltpu.roll(x, R + 31, 0)[16:16 + R]
        conv = taps[0:1] * before + taps[1:2] * x[16:16 + R] + taps[2:3] * after
        conv = postb[here, :].astype(F32) * conv
        act[here, pl.ds(al(T * F + own * Q, 128), Q)] = conv.astype(BF)
        return carry

    lax.fori_loop(0, M, attend, 0)

    for b in range(2):
        for k in range(1, M):
            send(act_at(b, c, j), act_at(b, c, j), base["act"] + b * M + j, g * M + lax.rem(j + k, M), c)
        send(act_at(b, c, j), act_at(b, c, j), base["act2"] + b * M + j, sp, peer)

    def gate(m, carry):
        here = pl.ds(al(m * R, 128), R)
        p = jnp.dot(normed[pl.ds(al(H + m * R, 64), R), :], wb[...], preferred_element_type=F32)
        gates[here, :] = jax.nn.sigmoid(p)
        return carry

    lax.fori_loop(0, M, gate, 0)

    for i in range(pl_.pieces):
        for half in range(T):
            arrived(wo_at(i, half), base["wo"] + i * T + half)
    wide = pl_.wide
    woa[...] = jnp.concatenate([wo[i, :, :wide] for i in range(pl_.pieces)], axis=1)
    woc[...] = jnp.concatenate([wo[i, :, wide:] for i in range(pl_.pieces)], axis=1)

    for b in range(2):
        for k in range(1, M):
            source = lax.rem(j + M - k, M)
            arrived(act_at(b, c, source), base["act"] + b * M + source)
            send(act_at(b, c, source), act_at(b, c, source), base["act2"] + b * M + source, sp, peer)
    for b in range(2):
        for k in range(M):
            arrived(act_at(b, peer, k), base["act2"] + b * M + k)

    for k in range(1, M + 1):
        m = lax.rem(j + k, M)
        here = pl.ds(al(m * R, 128), R)
        attn = jnp.dot(act[here, :T * F], woa[...], preferred_element_type=F32)
        conv = jnp.dot(act[here, T * F:], woc[...], preferred_element_type=F32)
        gg = gates[here, :]
        merged = (gg[:, :Q] * attn + gg[:, Q:] * conv).astype(BF)
        if k < M:
            mix[k] = merged
            send(mix.at[k], outb.at[j], base["out"] + j, g * M + m, c)
        else:
            o_ref[:, pl.ds(al(j * Q, 128), Q)] = merged
    for k in range(1, M):
        source = lax.rem(j + M - k, M)
        arrived(outb.at[source], base["out"] + source)
        o_ref[:, pl.ds(al(source * Q, 128), Q)] = outb[source]

    for copy, when in waits:
        if when is None:
            copy.wait_send()
        else:
            pl.when(when)(functools.partial(lambda item: item.wait_send(), copy))


def in_planes(
    plan, tokens, norm_gain, query_weight, key_weight, value_weight, conv_in_weight,
    pre_weight, post_weight, attn_gate_weight, conv_gate_weight, sink_logit, conv_taps,
    attn_out_weight, conv_out_weight,
):
    M, G, T = plan.members, plan.planes, plan.tp
    R, F, Q, ALL = plan.rows, plan.feat, plan.q, plan.all_rows
    D = plan.sp * plan.depth

    def packed(*weights):
        cut = [w.reshape(w.shape[0], M, -1).transpose(1, 0, 2) for w in weights]
        return jnp.concatenate(cut, axis=2)

    pa = packed(query_weight, key_weight, value_weight, conv_in_weight, pre_weight, post_weight)
    pb = packed(attn_gate_weight, conv_gate_weight)
    po = jnp.concatenate([attn_out_weight, conv_out_weight], axis=1)
    vmem = pl.BlockSpec(memory_space=pltpu.VMEM)
    span = ALL + 2 * WINDOW
    return pl.pallas_call(
        functools.partial(kernel, plan),
        out_shape=jax.ShapeDtypeStruct(tokens.shape, BF),
        in_specs=[vmem] * 5 + [pl.BlockSpec(memory_space=pltpu.SMEM), vmem],
        out_specs=vmem,
        scratch_shapes=[
            pltpu.VMEM((span, T * F), BF),
            pltpu.VMEM((span, T * F), BF),
            pltpu.VMEM((1, T * F), F32),
            pltpu.VMEM((D, pa.shape[2]), BF),
            pltpu.VMEM((D, pb.shape[2]), BF),
            pltpu.VMEM((plan.pieces, T * F, po.shape[1]), BF),
            pltpu.VMEM((T * F, Q), BF),
            pltpu.VMEM((T * F, Q), BF),
            pltpu.VMEM((ALL, Q), BF),
            pltpu.VMEM((span, 2 * Q), BF),
            pltpu.VMEM((ALL, Q), BF),
            pltpu.VMEM((ALL, 2 * T * F), BF),
            pltpu.VMEM((ALL, 2 * Q), F32),
            pltpu.VMEM((M, R, Q), BF),
            pltpu.VMEM((M, R, Q), BF),
            pltpu.SemaphoreType.DMA((16 * M + 4 * G + 16,)),
            pltpu.SemaphoreType.DMA((16 * M + 4 * G + 16,)),
            pltpu.SemaphoreType.DMA((4,)),
        ],
        compiler_params=pltpu.CompilerParams(
            collective_id=0, has_side_effects=True, vmem_limit_bytes=48 * 1024 * 1024
        ),
        name="mixer",
    )(tokens, norm_gain[None, :], pa, pb, po, sink_logit[None, :], conv_taps)


def per_device(*args):
    plan = Plan(lax.axis_size("sp"), lax.axis_size("tp"), args[0], args[2], args[3], args[12])
    if plan.fits():
        return in_planes(plan, *args)
    return gathered_everywhere(*args)


def solution(mesh):
    return jax.shard_map(
        per_device,
        mesh=mesh,
        in_specs=(
            P("sp", "tp"),
            P("tp"),
            P("sp", "tp"),
            P("sp", "tp"),
            P("sp", "tp"),
            P("sp", "tp"),
            P("sp", "tp"),
            P("sp", "tp"),
            P("sp", "tp"),
            P("sp", "tp"),
            P("tp"),
            P(None, "tp"),
            P("tp", "sp"),
            P("tp", "sp"),
        ),
        out_specs=P("sp", "tp"),
        check_vma=False,
    )
```
